32 devices in a mesh: kv: 8 (over z, x), tp: 4 (over y, core).
Axes of the slice: x: 2, y: 2, z: 4, core: 2. Of those that a mesh axis runs over, the one named last changes fastest.
Arguments:
- tokens: bfloat16 [18, 4096], P(None, ('kv', 'tp')), may hold values from -12.2 to 12.2
- norm_gains: float32 [6, 4096], replicated, may hold values from 0.1 to 1.9
- first_gate: bfloat16 [4096, 11264], P(None, ('kv', 'tp')), may hold values from -0.09375 to 0.09375
- first_lift: bfloat16 [4096, 11264], P(None, ('kv', 'tp')), may hold values from -0.09375 to 0.09375
- first_down: bfloat16 [11264, 4096], P(('kv', 'tp')), may hold values from -0.109375 to 0.109375
- query_weight: bfloat16 [4096, 4096], P('kv', 'tp'), may hold values from -0.09375 to 0.09375
- key_weight: bfloat16 [4096, 4096], P('kv', 'tp'), may hold values from -0.09375 to 0.09375
- value_weight: bfloat16 [4096, 4096], P('kv', 'tp'), may hold values from -0.09375 to 0.09375
- forget_weight: bfloat16 [4096, 64], P(None, 'tp'), may hold values from -0.25 to 0.25
- output_weight: bfloat16 [4096, 4096], P('tp', 'kv'), may hold values from -0.09375 to 0.09375
- second_gate: bfloat16 [4096, 11264], P(None, ('kv', 'tp')), may hold values from -0.09375 to 0.09375
- second_lift: bfloat16 [4096, 11264], P(None, ('kv', 'tp')), may hold values from -0.09375 to 0.09375
- second_down: bfloat16 [11264, 4096], P(('kv', 'tp')), may hold values from -0.109375 to 0.109375
- cache_keys: bfloat16 [18, 2048, 4096], P(None, 'kv', 'tp'), may hold values from -457 to 457
- cache_values: bfloat16 [18, 2048, 4096], P(None, 'kv', 'tp'), may hold values from -6 to 6
- cache_decay: float32 [18, 64, 2048], P(None, 'tp', 'kv'), may hold values from -2500 to 0, as said below
Outputs:
- layer_out: bfloat16 [18, 4096], P(None, ('kv', 'tp'))
The draws below stay inside these ranges and needn't reach their ends.
Inputs may be any that keep to these rules, and one draw needn't show every extreme that they name: `cache_decay`: each entry is a sum of log forget gates, each at most zero, of the later cached positions of the same sequence and head, so entries never fall along positions and the last is zero.
All inputs are finite; a program needn't handle non-finite values.
Results may differ from the reference program's by a relative error of at most 0.025.
Values may be sent and summed in bfloat16 or wider, within the bound.
A program may use at most 128 MiB of HBM per device.

```python
import math
import jax
import jax.numpy as jnp
from jax import lax

D = 4096
HEADS = 64
HD = 64
FF = 11264
SEQUENCE_COUNT = 18
POS_DEV = 256
CACHED_POSITIONS = 2048
KW = 4096
N_KV = 8
N_TP = 4


def draw_tokens(key, part):
    first_key, second_key = jax.random.split(key)
    column_ramp = jnp.arange(D, dtype=jnp.float32) / (D - 1) - 0.5
    sample = jnp.clip(jax.random.normal(first_key, (SEQUENCE_COUNT, D), jnp.float32), -5.0, 5.0)
    column_scale = 3.0 ** column_ramp
    roughness = jax.random.uniform(second_key, (1, D), jnp.float32, 0.6, 1.4)
    return (sample * column_scale[None, :] * roughness).astype(jnp.bfloat16)


def draw_cache_keys(key, part):
    random_key_split = jax.random.split(key, 1)
    sample = jnp.clip(jax.random.normal(random_key_split[0], (SEQUENCE_COUNT, CACHED_POSITIONS, KW), jnp.float32), -5.0, 5.0)
    return sample.astype(jnp.bfloat16)


def draw_cache_decay(key, part):
    random_key_split = jax.random.split(key, 7)
    full_shape = (SEQUENCE_COUNT, HEADS, CACHED_POSITIONS)
    slow_share = 0.5
    slow_heads = jax.random.uniform(random_key_split[0], (SEQUENCE_COUNT, HEADS, 1), jnp.float32) < slow_share
    slow_total = jax.random.uniform(random_key_split[1], (SEQUENCE_COUNT, HEADS, 1), jnp.float32, 0.3, 0.8)
    fast_rate = jnp.exp(jax.random.uniform(random_key_split[2], (SEQUENCE_COUNT, HEADS, 1), jnp.float32, math.log(0.03), math.log(0.1)))
    baseline_rate = jnp.where(slow_heads, slow_total / CACHED_POSITIONS, fast_rate)
    block_count = CACHED_POSITIONS // POS_DEV
    block_multiplier = jnp.exp(jax.random.uniform(random_key_split[3], (SEQUENCE_COUNT, HEADS, block_count, 1), jnp.float32, math.log(0.5), math.log(1.5)))
    block_multiplier = jnp.broadcast_to(block_multiplier, (SEQUENCE_COUNT, HEADS, block_count, POS_DEV)).reshape(full_shape)
    random_noise = jax.random.uniform(random_key_split[4], full_shape, jnp.float32, 0.2, 1.8)
    spike_position = jax.random.randint(random_key_split[5], (SEQUENCE_COUNT, 2), 0, CACHED_POSITIONS)
    spike_penalty = jax.random.uniform(random_key_split[6], (SEQUENCE_COUNT, 2), jnp.float32, 0.2, 0.4)
    position_index = jnp.arange(CACHED_POSITIONS)
    sudden_spike = jnp.sum(jnp.where(position_index[None, None, :] == spike_position[:, :, None], jnp.log(1.0 - spike_penalty)[:, :, None], 0.0), axis=1)
    gate_values = -baseline_rate * block_multiplier * random_noise + sudden_spike[:, None, :]
    running = jnp.cumsum(gate_values, axis=2)
    return running[:, :, -1:] - running


def spiked(entries, own_key, source, target, parts, factor):
    owner, partner = [(jnp.arange(entries.shape[axis_at]) // (entries.shape[axis_at] // parts)).reshape([-1 if axis == axis_at else 1 for axis in range(entries.ndim)]) for axis_at in (source, target)]
    chosen = jax.random.permutation(own_key, parts)[partner]
    strong = (owner == chosen) | (owner == (partner + parts // 2) % parts)
    return jnp.where(strong, factor * entries, entries)


def block_scale(key, dims, shards, smallest, top_value):
    factor_of, own = 1.0, jax.random.fold_in(key, 6)
    for axis_at, blocks in shards:
        heights = jnp.exp(jax.random.uniform(jax.random.fold_in(own, axis_at), (blocks,), jnp.float32, smallest / len(shards), top_value / len(shards)))
        factor_of = factor_of * jnp.repeat(heights, dims[axis_at] // blocks).reshape([-1 if axis == axis_at else 1 for axis in range(len(dims))])
    return factor_of


def centred(key, dims, deviation, bound, shards=(), held_as=jnp.bfloat16):
    loudness = block_scale(key, dims, shards, -0.22, 0.18) if shards else 1.0
    drawn = jax.random.normal(key, dims, jnp.float32) * deviation * loudness
    return jnp.minimum(jnp.maximum(drawn, -bound), bound).astype(held_as)


def gaussian_with(rng, shape, width, limit, pieces, heavy, kind=jnp.bfloat16):
    entries = width * jax.random.normal(rng, shape, jnp.float32)
    if pieces:
        entries = entries * block_scale(rng, shape, pieces, -0.22, 0.18)
    return jnp.clip(spiked(entries, jax.random.fold_in(rng, 3), *heavy), -limit, limit).astype(kind)


def setup_inputs(seed: int = 0) -> dict:
    streams_of = jax.random.split(jax.random.key(seed), 17)
    return {
        "tokens": draw_tokens(jax.random.fold_in(streams_of[16], 71), 0),
        "norm_gains": jnp.clip(1.0 + 0.18 * jax.random.normal(streams_of[1], (6, D), jnp.float32), 0.1, 1.9),
        "first_gate": centred(streams_of[2], (D, FF), D ** -0.5, 0.09375, ((1, 32),)),
        "first_lift": centred(streams_of[3], (D, FF), D ** -0.5, 0.09375, ((1, 32),)),
        "first_down": gaussian_with(streams_of[4], (FF, D), FF ** -0.5, 0.109375, ((0, 32),), (0, 1, 32, 2.75)),
        "query_weight": centred(streams_of[5], (D, KW), D ** -0.5, 0.09375, ((0, 8), (1, 4))),
        "key_weight": centred(streams_of[6], (D, KW), D ** -0.5, 0.09375, ((0, 8), (1, 4))),
        "value_weight": centred(streams_of[7], (D, KW), D ** -0.5, 0.09375, ((0, 8), (1, 4))),
        "forget_weight": centred(streams_of[8], (D, HEADS), (D // 9) ** -0.5, 0.25, ((1, 4),)),
        "output_weight": centred(streams_of[9], (KW, D), KW ** -0.5, 0.09375, ((0, 4), (1, 8))),
        "second_gate": centred(streams_of[10], (D, FF), D ** -0.5, 0.09375, ((1, 32),)),
        "second_lift": centred(streams_of[11], (D, FF), D ** -0.5, 0.09375, ((1, 32),)),
        "second_down": gaussian_with(streams_of[12], (FF, D), FF ** -0.5, 0.109375, ((0, 32),), (0, 1, 32, 2.75)),
        "cache_keys": draw_cache_keys(jax.random.fold_in(streams_of[16], 71), 0),
        "cache_values": centred(streams_of[14], (SEQUENCE_COUNT, CACHED_POSITIONS, KW), 1.0, 6.0, ((1, 8), (2, 4))),
        "cache_decay": draw_cache_decay(jax.random.fold_in(streams_of[16], 71), 0),
    }


epsilon = 1e-06

def root_norm(values, norm_gain):
    return values * lax.rsqrt(lax.optimization_barrier(jnp.mean(values * values, axis=-1, keepdims=True)) + epsilon) * norm_gain

def settle(values):
    return lax.optimization_barrier(values.astype(jnp.bfloat16)).astype(jnp.float32)

def gated_half(stream, pre_gain, post_gain, gate_matrix, lift_matrix, down_matrix):
    normed = root_norm(stream, pre_gain).astype(jnp.bfloat16)
    gate_part = jnp.dot(normed, gate_matrix, preferred_element_type=jnp.float32)
    lift_part = jnp.dot(normed, lift_matrix, preferred_element_type=jnp.float32)
    active = (jax.nn.silu(gate_part) * lift_part).astype(jnp.bfloat16)
    branch = settle(jnp.dot(active, down_matrix, preferred_element_type=jnp.float32))
    return stream + 0.5 * root_norm(branch, post_gain)

def attend_one(inputs):
    queries, key_new, value_new, forget, key_rows, value_rows, decay_rows = inputs
    score_scale = HD ** (-0.5)
    query_heads = queries.reshape(HEADS, HD).astype(jnp.float32)
    key_heads = key_rows.reshape(N_KV, POS_DEV, HEADS, HD).astype(jnp.float32)
    value_heads = value_rows.reshape(N_KV, POS_DEV, HEADS, HD).astype(jnp.float32)
    scores = jnp.einsum('hd,nphd->hnp', query_heads, key_heads) * score_scale
    scores = scores + forget[:, None, None] + decay_rows.reshape(HEADS, N_KV, POS_DEV)
    block_peak = lax.optimization_barrier(jnp.max(scores, axis=2))
    raised = jnp.exp(scores - block_peak[:, :, None])
    totals = lax.optimization_barrier(jnp.sum(raised, axis=2))
    weights = settle(raised)
    block_out = settle(jnp.einsum('hnp,nphd->hnd', weights, value_heads) / totals[:, :, None])
    own_score = lax.optimization_barrier(jnp.sum(query_heads * key_new.reshape(HEADS, HD).astype(jnp.float32), axis=1)) * score_scale
    summit = jnp.maximum(own_score, lax.optimization_barrier(jnp.max(block_peak, axis=1)))
    block_weight = totals * jnp.exp(block_peak - summit[:, None])
    own_weight = jnp.exp(own_score - summit)
    summed = lax.optimization_barrier(jnp.sum(block_weight[:, :, None] * block_out, axis=1))
    summed = summed + own_weight[:, None] * value_new.reshape(HEADS, HD).astype(jnp.float32)
    joined = summed / (lax.optimization_barrier(jnp.sum(block_weight, axis=1)) + own_weight)[:, None]
    return joined.astype(jnp.bfloat16).reshape(HEADS * HD)

def reference(tokens, norm_gains, first_gate, first_lift, first_down, query_weight, key_weight, value_weight, forget_weight, output_weight, second_gate, second_lift, second_down, cache_keys, cache_values, cache_decay):
    stream = tokens.astype(jnp.float32)
    middle = gated_half(stream, norm_gains[0], norm_gains[1], first_gate, first_lift, first_down)
    normed = root_norm(middle, norm_gains[2]).astype(jnp.bfloat16)
    queries = jnp.dot(normed, query_weight, preferred_element_type=jnp.float32).astype(jnp.bfloat16)
    key_new = jnp.dot(normed, key_weight, preferred_element_type=jnp.float32).astype(jnp.bfloat16)
    value_new = jnp.dot(normed, value_weight, preferred_element_type=jnp.float32).astype(jnp.bfloat16)
    forget = jax.nn.log_sigmoid(jnp.dot(normed, forget_weight, preferred_element_type=jnp.float32))
    attended = lax.map(attend_one, (queries, key_new, value_new, forget, cache_keys, cache_values, cache_decay))
    seq_count = tokens.shape[0]
    head_groups = attended.reshape(seq_count, N_TP, KW // N_TP).astype(jnp.float32)
    weight_groups = output_weight.reshape(N_TP, KW // N_TP, D).astype(jnp.float32)
    partials = settle(jnp.einsum('bnk,nkd->bnd', head_groups, weight_groups))
    mixed_rows = settle(lax.optimization_barrier(jnp.sum(partials, axis=1)))
    after_mix = middle + root_norm(mixed_rows, norm_gains[3])
    layer_out = gated_half(after_mix, norm_gains[4], norm_gains[5], second_gate, second_lift, second_down)
    return layer_out.astype(jnp.bfloat16)
```

```python
import functools

import jax
import jax.numpy as jnp
from jax import lax
from jax.experimental import pallas as pl
from jax.experimental.pallas import tpu as pltpu
from jax.sharding import PartitionSpec as P

HD = 64


epsilon = 1e-06


def root_norm(values, norm_gain):
    return (
        values * lax.rsqrt(jnp.mean(values * values, axis=-1, keepdims=True) + epsilon) * norm_gain
    )


def settle(values):
    return lax.optimization_barrier(values.astype(jnp.bfloat16)).astype(jnp.float32)


def gated_terms(stream, pre_gain, gate_matrix, lift_matrix, down_matrix):
    normed = root_norm(stream, pre_gain).astype(jnp.bfloat16)
    gate_part = jnp.dot(normed, gate_matrix, preferred_element_type=jnp.float32)
    lift_part = jnp.dot(normed, lift_matrix, preferred_element_type=jnp.float32)
    active = (jax.nn.silu(gate_part) * lift_part).astype(jnp.bfloat16)
    return jnp.dot(active, down_matrix, preferred_element_type=jnp.float32)


def branch_total(partial_value):
    summed = lax.psum(partial_value, ("kv", "tp"))
    return summed


def spread_heads(per_head):
    return jnp.repeat(per_head, HD, axis=-1)


def absorb(carried, pieces):
    summit, weight_sum, out_sum = carried
    piece_peak, piece_total, piece_out = pieces
    new_summit = jnp.maximum(summit, jnp.max(piece_peak, axis=0))
    kept_share = jnp.exp(summit - new_summit)
    piece_weight = piece_total * jnp.exp(piece_peak - new_summit[None])
    weight_sum = weight_sum * kept_share + jnp.sum(piece_weight, axis=0)
    out_sum = out_sum * spread_heads(kept_share) + jnp.sum(
        spread_heads(piece_weight) * piece_out, axis=0
    )
    return (new_summit, weight_sum, out_sum)


def body(
    tokens,
    norm_gains,
    first_gate,
    first_lift,
    first_down,
    query_weight,
    key_weight,
    value_weight,
    forget_weight,
    output_weight,
    second_gate,
    second_lift,
    second_down,
    cache_keys,
    cache_values,
    cache_decay,
):
    seq_count = tokens.shape[0]
    own_width = tokens.shape[1]
    own_start = lax.axis_index(("kv", "tp")) * own_width
    stream = lax.all_gather(tokens, ("kv", "tp"), axis=1, tiled=True).astype(jnp.float32)
    first_sum = branch_total(gated_terms(stream, norm_gains[0], first_gate, first_lift, first_down))
    first_branch = settle(first_sum)
    middle = stream + 0.5 * root_norm(first_branch, norm_gains[1])
    normed = root_norm(middle, norm_gains[2]).astype(jnp.bfloat16)
    block_rows = query_weight.shape[0]
    feature_block = lax.dynamic_slice_in_dim(
        normed, lax.axis_index("kv") * block_rows, block_rows, 1
    )
    query_part = jnp.dot(feature_block, query_weight, preferred_element_type=jnp.float32)
    key_part = jnp.dot(feature_block, key_weight, preferred_element_type=jnp.float32)
    value_part = jnp.dot(feature_block, value_weight, preferred_element_type=jnp.float32)
    queries, key_new, value_new = (
        lax.psum(query_part.astype(jnp.bfloat16), "kv").astype(jnp.float32),
        lax.psum(key_part.astype(jnp.bfloat16), "kv").astype(jnp.float32),
        lax.psum(value_part.astype(jnp.bfloat16), "kv").astype(jnp.float32),
    )
    queries = queries.astype(jnp.bfloat16)
    key_new = key_new.astype(jnp.bfloat16)
    value_new = value_new.astype(jnp.bfloat16)
    forget = jax.nn.log_sigmoid(jnp.dot(normed, forget_weight, preferred_element_type=jnp.float32))
    head_count = forget_weight.shape[1]
    position_index = cache_keys.shape[1]
    score_scale = HD ** (-0.5)
    query_heads = queries.reshape(seq_count, head_count, HD)
    key_heads = cache_keys.reshape(seq_count, position_index, head_count, HD)
    value_heads = cache_values.reshape(seq_count, position_index, head_count, HD)
    scores = (
        jnp.einsum("bhd,bphd->bhp", query_heads, key_heads, preferred_element_type=jnp.float32)
        * score_scale
    )
    scores = scores + forget[:, :, None] + cache_decay
    block_peak = jnp.max(scores, axis=2)
    raised = jnp.exp(scores - block_peak[:, :, None])
    block_total = jnp.sum(raised, axis=2)
    weighted = jnp.einsum(
        "bhp,bphd->bhd",
        raised.astype(jnp.bfloat16),
        value_heads,
        preferred_element_type=jnp.float32,
    )
    block_out = settle(weighted / block_total[:, :, None]).reshape(seq_count, head_count * HD)
    own_score = (
        jnp.einsum(
            "bhd,bhd->bh",
            query_heads,
            key_new.reshape(seq_count, head_count, HD),
            preferred_element_type=jnp.float32,
        )
        * score_scale
    )
    own_part = (own_score, jnp.ones_like(own_score), value_new.astype(jnp.float32))
    summit, weight_sum, out_sum = absorb(
        own_part,
        (
            lax.all_gather(block_peak[None].astype(jnp.bfloat16), "kv", axis=0, tiled=True).astype(
                jnp.float32
            ),
            lax.all_gather(block_total[None].astype(jnp.bfloat16), "kv", axis=0, tiled=True).astype(
                jnp.float32
            ),
            lax.all_gather(block_out[None].astype(jnp.bfloat16), "kv", axis=0, tiled=True).astype(
                jnp.float32
            ),
        ),
    )
    attended = (out_sum / spread_heads(weight_sum)).astype(jnp.bfloat16)
    projected = settle(jnp.dot(attended, output_weight, preferred_element_type=jnp.float32))
    mixed_block = lax.psum(projected.astype(jnp.bfloat16), "tp")
    mixed_rows = lax.all_gather(mixed_block, "kv", axis=1, tiled=True).astype(jnp.float32)
    after_mix = middle + root_norm(mixed_rows, norm_gains[3])
    second_sum = branch_total(
        gated_terms(after_mix, norm_gains[4], second_gate, second_lift, second_down)
    )
    own_rows = lax.dynamic_slice_in_dim(after_mix, own_start, own_width, 1)
    second_branch = lax.dynamic_slice_in_dim(
        root_norm(settle(second_sum), norm_gains[5]), own_start, own_width, 1
    )
    return (own_rows + 0.5 * second_branch).astype(jnp.bfloat16)


MESH = pl.DeviceIdType.MESH
F32 = jnp.float32
BF16 = jnp.bfloat16


def wide_dot(a, b):
    return lax.dot_general(a, b, (((1,), (1,)), ((), ())), preferred_element_type=F32)


def fused_kernel(n_kv, n_tp, *refs):
    n = n_kv * n_tp
    (tokens, gains, *hbm_refs) = refs[:16]
    out = refs[16]
    vmem_refs = refs[17:31]
    (
        x2d, stage, nrm, mid, part_sum, q2d, o2d, l2d,
        xbuf, send_all, recv_all, own_all, bbuf, mbuf, recv_two, tbuf,
        send_qkv, recv_qkv, own_kv, qbuf, send_part, recv_part,
        send_lse, recv_lse, abuf, send_tp, recv_tp,
        load_sem, all_send, all_recv, kv_send, kv_recv, tp_send, tp_recv,
    ) = refs[31:]
    (
        g1, l1, d1, wq, wk, wv, wf, wo, g2, l2, d2, ck, cv, cd
    ) = vmem_refs
    rows, c = tokens.shape
    depth = n * c
    kv = lax.axis_index("kv")
    tp = lax.axis_index("tp")
    me = kv * n_tp + tp

    order = (0, 1, 2, 3, 4, 5, 6, 11, 13, 12, 7, 8, 9, 10)
    loads = [
        pltpu.make_async_copy(hbm_refs[i], vmem_refs[i], load_sem.at[i]) for i in range(14)
    ]
    for i in order:
        loads[i].start()

    barrier = pltpu.get_barrier_semaphore()

    @pl.loop(1, n)
    def _(k):
        peer = lax.rem(me + k, n)
        pl.semaphore_signal(
            barrier, inc=1, device_id=(lax.div(peer, n_tp), lax.rem(peer, n_tp)),
            device_id_type=MESH,
        )

    pl.semaphore_wait(barrier, n - 1)

    def group(axis):
        if axis == "all":
            return n, me, lambda p: (lax.div(p, n_tp), lax.rem(p, n_tp)), all_send, all_recv
        if axis == "kv":
            return n_kv, kv, lambda p: (p, tp), kv_send, kv_recv
        return n_tp, tp, lambda p: (kv, p), tp_send, tp_recv

    def remote(src, dst, slot, axis, which, peer, index):
        size, here, place, send_sem, recv_sem = group(axis)
        return pltpu.make_async_remote_copy(
            src_ref=src, dst_ref=dst.at[slot],
            send_sem=send_sem.at[which, peer], recv_sem=recv_sem.at[which, index],
            device_id=place(peer), device_id_type=MESH,
        )

    def exchange(axis, pairs):
        size, here = group(axis)[:2]

        @pl.loop(1, size)
        def _(k):
            peer = lax.rem(here + k, size)
            for src, dst, which, scattered in pairs:
                remote(
                    src.at[peer] if scattered else src, dst, here, axis, which, peer, here
                ).start()

        for src, dst, which, scattered in pairs:
            dst[here] = src[here] if scattered else src[...]

        @pl.loop(1, size)
        def _(k):
            peer = lax.rem(here + k, size)
            for src, dst, which, scattered in pairs:
                remote(
                    src.at[peer] if scattered else src, dst, peer, axis, which, peer, peer
                ).wait()

    def flatten(buf, target, count):
        for i in range(count):
            target[:, i * c : (i + 1) * c] = buf[i].astype(target.dtype)

    def branch(pre_ref, gate, lift, down, first_load):
        for i in range(3):
            loads[first_load + i].wait()
        hidden = gate.shape[0]
        step = c * max(1, min(4, n))

        def up(k, carry):
            a, b = carry
            ds = pl.ds(pl.multiple_of(k * step, c), step)
            v = pre_ref[:, ds]
            a = a + wide_dot(v, gate[:, ds])
            b = b + wide_dot(v, lift[:, ds])
            return a, b

        zero = jnp.zeros((rows, hidden), F32)
        a, b = lax.fori_loop(0, depth // step, up, (zero, zero))
        active = (a / (1.0 + jnp.exp(-a)) * b).astype(BF16)
        group_size = step // c

        @pl.loop(0, depth // step)
        def _(k):
            ds = pl.ds(pl.multiple_of(k * step, c), step)
            y = jnp.dot(active, down[:, ds], preferred_element_type=F32).astype(BF16)
            for j in range(group_size):
                send_all[k * group_size + j] = y[:, j * c : (j + 1) * c]

    def total(buf, count):
        acc = buf[0].astype(F32)
        for i in range(1, count):
            acc = acc + buf[i].astype(F32)
        return acc

    exchange("all", [(tokens, xbuf, 0, False)])
    flatten(xbuf, x2d, n)
    nrm[...] = root_norm(x2d[...], gains[0:1, :]).astype(BF16)
    branch(nrm, g1, l1, d1, 0)
    exchange("all", [(send_all, recv_all, 1, True)])
    own_all[...] = total(recv_all, n).astype(BF16)
    exchange("all", [(own_all, bbuf, 2, False)])
    flatten(bbuf, stage, n)
    middle = x2d[...] + 0.5 * root_norm(stage[...], gains[1:2, :])
    mid[...] = middle
    nrm[...] = root_norm(middle, gains[2:3, :]).astype(BF16)

    for i in (3, 4, 5, 6):
        loads[i].wait()
    block_rows = wq.shape[0]
    block = nrm[:, pl.ds(pl.multiple_of(kv * block_rows, c), block_rows)]
    for i, w in enumerate((wq, wk, wv)):
        y = jnp.dot(block, w[...], preferred_element_type=F32).astype(BF16)
        for j in range(n_kv):
            send_qkv[j, i] = y[:, j * c : (j + 1) * c]
    forget_t = jax.nn.log_sigmoid(wide_dot(wf[...], nrm[...]))
    exchange("kv", [(send_qkv, recv_qkv, 0, True)])
    qkv = total(recv_qkv, n_kv).astype(BF16)
    own_kv[...] = qkv[0]
    exchange("kv", [(own_kv, qbuf, 1, False)])
    flatten(qbuf, q2d, n_kv)

    for i in (11, 12, 13):
        loads[i].wait()
    heads = wf.shape[0]
    width = heads * HD
    scale = HD ** (-0.5)
    head_of = lax.broadcasted_iota(jnp.int32, (heads, width), 1) // HD
    mask = head_of == lax.broadcasted_iota(jnp.int32, (heads, width), 0)

    for b in range(rows):
        q = jnp.where(mask, q2d[b : b + 1, :], 0.0).astype(BF16)
        s = wide_dot(q, ck[b]) * scale + forget_t[:, b : b + 1] + cd[b]
        peak = jnp.max(s, axis=1, keepdims=True)
        e = jnp.exp(s - peak)
        sums = jnp.sum(e, axis=1, keepdims=True)
        o = jnp.dot(e.astype(BF16), cv[b], preferred_element_type=F32) / sums
        lse = peak + jnp.log(sums)
        o2d[b : b + 1, :] = jnp.sum(jnp.where(mask, o, 0.0), axis=0, keepdims=True)
        l2d[b : b + 1, :] = jnp.sum(jnp.where(mask, lse, 0.0), axis=0, keepdims=True)

    for j in range(n_kv):
        send_part[j] = o2d[:, j * c : (j + 1) * c].astype(BF16)
        send_lse[j] = l2d[:, j * c : (j + 1) * c]
    exchange("kv", [(send_part, recv_part, 2, True), (send_lse, recv_lse, 3, True)])
    qk = qkv[0].astype(F32) * qkv[1].astype(F32)
    lane_head = lax.broadcasted_iota(jnp.int32, (rows, c), 1) // HD
    own = jnp.zeros((rows, c), F32)
    for h in range(c // HD):
        mine = lane_head == h
        own = jnp.where(
            mine, jnp.sum(jnp.where(mine, qk, 0.0), axis=1, keepdims=True) * scale, own
        )
    top = own
    for j in range(n_kv):
        top = jnp.maximum(top, recv_lse[j])
    weight = jnp.exp(own - top)
    value = weight * qkv[2].astype(F32)
    for j in range(n_kv):
        w = jnp.exp(recv_lse[j] - top)
        weight = weight + w
        value = value + w * recv_part[j].astype(F32)
    own_kv[...] = (value / weight).astype(BF16)
    exchange("kv", [(own_kv, abuf, 4, False)])
    flatten(abuf, q2d, n_kv)
    loads[7].wait()
    y = jnp.dot(q2d[...].astype(BF16), wo[...], preferred_element_type=F32).astype(BF16)
    for j in range(n_tp):
        send_tp[j] = y[:, j * c : (j + 1) * c]
    exchange("tp", [(send_tp, recv_tp, 0, True)])
    own_all[...] = total(recv_tp, n_tp).astype(BF16)
    exchange("all", [(own_all, mbuf, 3, False)])
    flatten(mbuf, stage, n)
    after = mid[...] + root_norm(stage[...], gains[3:4, :])
    mid[...] = after
    nrm[...] = root_norm(after, gains[4:5, :]).astype(BF16)
    branch(nrm, g2, l2, d2, 8)
    exchange("all", [(send_all, recv_two, 4, True)])
    last = total(recv_two, n).astype(BF16)
    own_all[...] = last
    exchange("all", [(own_all, tbuf, 5, False)])
    squares = jnp.zeros((rows, c), F32)
    for i in range(n):
        v = tbuf[i].astype(F32)
        squares = squares + v * v
    inv = lax.rsqrt(jnp.sum(squares, axis=1, keepdims=True) / depth + epsilon)
    here = pl.ds(pl.multiple_of(me * c, c), c)
    out[...] = (mid[:, here] + 0.5 * (last.astype(F32) * inv * gains[5:6, here])).astype(BF16)


def layer(n_kv, n_tp, *args):
    tokens = args[0]
    rows, c = tokens.shape
    n = n_kv * n_tp
    if c % 128 or args[5].shape[1] != n_kv * c or args[9].shape[1] != n_tp * c:
        return body(*args)
    depth = n * c
    width = args[8].shape[1] * HD
    args = [a.T if i in (2, 3, 8, 10, 11) else a for i, a in enumerate(args)]
    vmem = pltpu.VMEM
    chunk = (rows, c)
    dma = pltpu.SemaphoreType.DMA
    scratch = [vmem(a.shape, a.dtype) for a in args[2:]]
    scratch += [
        vmem((rows, depth), F32),
        vmem((rows, depth), F32),
        vmem((rows, depth), BF16),
        vmem((rows, depth), F32),
        vmem((8, 128), F32),
        vmem((rows, width), F32),
        vmem((rows, width), F32),
        vmem((rows, width), F32),
        vmem((n, *chunk), BF16),
        vmem((n, *chunk), BF16),
        vmem((n, *chunk), BF16),
        vmem(chunk, BF16),
        vmem((n, *chunk), BF16),
        vmem((n, *chunk), BF16),
        vmem((n, *chunk), BF16),
        vmem((n, *chunk), BF16),
        vmem((n_kv, 3, *chunk), BF16),
        vmem((n_kv, 3, *chunk), BF16),
        vmem(chunk, BF16),
        vmem((n_kv, *chunk), BF16),
        vmem((n_kv, *chunk), BF16),
        vmem((n_kv, *chunk), BF16),
        vmem((n_kv, *chunk), F32),
        vmem((n_kv, *chunk), F32),
        vmem((n_kv, *chunk), BF16),
        vmem((n_tp, *chunk), BF16),
        vmem((n_tp, *chunk), BF16),
        dma((14,)),
        dma((6, n)),
        dma((6, n)),
        dma((5, n_kv)),
        dma((5, n_kv)),
        dma((1, n_tp)),
        dma((1, n_tp)),
    ]
    anywhere = pl.BlockSpec(memory_space=pl.ANY)
    inside = pl.BlockSpec(memory_space=pltpu.VMEM)
    return pl.pallas_call(
        functools.partial(fused_kernel, n_kv, n_tp),
        out_shape=jax.ShapeDtypeStruct((rows, c), BF16),
        in_specs=[inside, inside] + [anywhere] * 14,
        out_specs=inside,
        scratch_shapes=scratch,
        compiler_params=pltpu.CompilerParams(
            collective_id=0, has_side_effects=True, vmem_limit_bytes=66 * 1000 * 1000
        ),
    )(*args)


def solution(mesh):
    return jax.shard_map(
        functools.partial(layer, mesh.shape["kv"], mesh.shape["tp"]),
        mesh=mesh,
        in_specs=(
            P(None, ("kv", "tp")),
            P(),
            P(None, ("kv", "tp")),
            P(None, ("kv", "tp")),
            P(("kv", "tp"), None),
            P("kv", "tp"),
            P("kv", "tp"),
            P("kv", "tp"),
            P(None, "tp"),
            P("tp", "kv"),
            P(None, ("kv", "tp")),
            P(None, ("kv", "tp")),
            P(("kv", "tp"), None),
            P(None, "kv", "tp"),
            P(None, "kv", "tp"),
            P(None, "tp", "kv"),
        ),
        out_specs=P(None, ("kv", "tp")),
        check_vma=False,
    )
```

```python
import functools

import jax
import jax.numpy as jnp
from jax import lax
from jax.experimental import pallas as pl
from jax.experimental.pallas import tpu as pltpu
from jax.sharding import PartitionSpec as P

HD = 64


epsilon = 1e-06


def root_norm(values, norm_gain):
    return (
        values * lax.rsqrt(jnp.mean(values * values, axis=-1, keepdims=True) + epsilon) * norm_gain
    )


def settle(values):
    return lax.optimization_barrier(values.astype(jnp.bfloat16)).astype(jnp.float32)


def gated_terms(stream, pre_gain, gate_matrix, lift_matrix, down_matrix):
    normed = root_norm(stream, pre_gain).astype(jnp.bfloat16)
    gate_part = jnp.dot(normed, gate_matrix, preferred_element_type=jnp.float32)
    lift_part = jnp.dot(normed, lift_matrix, preferred_element_type=jnp.float32)
    active = (jax.nn.silu(gate_part) * lift_part).astype(jnp.bfloat16)
    return jnp.dot(active, down_matrix, preferred_element_type=jnp.float32)


def branch_total(partial_value):
    summed = lax.psum(partial_value, ("kv", "tp"))
    return summed


def spread_heads(per_head):
    return jnp.repeat(per_head, HD, axis=-1)


def absorb(carried, pieces):
    summit, weight_sum, out_sum = carried
    piece_peak, piece_total, piece_out = pieces
    new_summit = jnp.maximum(summit, jnp.max(piece_peak, axis=0))
    kept_share = jnp.exp(summit - new_summit)
    piece_weight = piece_total * jnp.exp(piece_peak - new_summit[None])
    weight_sum = weight_sum * kept_share + jnp.sum(piece_weight, axis=0)
    out_sum = out_sum * spread_heads(kept_share) + jnp.sum(
        spread_heads(piece_weight) * piece_out, axis=0
    )
    return (new_summit, weight_sum, out_sum)


def body(
    tokens,
    norm_gains,
    first_gate,
    first_lift,
    first_down,
    query_weight,
    key_weight,
    value_weight,
    forget_weight,
    output_weight,
    second_gate,
    second_lift,
    second_down,
    cache_keys,
    cache_values,
    cache_decay,
):
    seq_count = tokens.shape[0]
    own_width = tokens.shape[1]
    own_start = lax.axis_index(("kv", "tp")) * own_width
    stream = lax.all_gather(tokens, ("kv", "tp"), axis=1, tiled=True).astype(jnp.float32)
    first_sum = branch_total(gated_terms(stream, norm_gains[0], first_gate, first_lift, first_down))
    first_branch = settle(first_sum)
    middle = stream + 0.5 * root_norm(first_branch, norm_gains[1])
    normed = root_norm(middle, norm_gains[2]).astype(jnp.bfloat16)
    block_rows = query_weight.shape[0]
    feature_block = lax.dynamic_slice_in_dim(
        normed, lax.axis_index("kv") * block_rows, block_rows, 1
    )
    query_part = jnp.dot(feature_block, query_weight, preferred_element_type=jnp.float32)
    key_part = jnp.dot(feature_block, key_weight, preferred_element_type=jnp.float32)
    value_part = jnp.dot(feature_block, value_weight, preferred_element_type=jnp.float32)
    queries, key_new, value_new = (
        lax.psum(query_part.astype(jnp.bfloat16), "kv").astype(jnp.float32),
        lax.psum(key_part.astype(jnp.bfloat16), "kv").astype(jnp.float32),
        lax.psum(value_part.astype(jnp.bfloat16), "kv").astype(jnp.float32),
    )
    queries = queries.astype(jnp.bfloat16)
    key_new = key_new.astype(jnp.bfloat16)
    value_new = value_new.astype(jnp.bfloat16)
    forget = jax.nn.log_sigmoid(jnp.dot(normed, forget_weight, preferred_element_type=jnp.float32))
    head_count = forget_weight.shape[1]
    position_index = cache_keys.shape[1]
    score_scale = HD ** (-0.5)
    query_heads = queries.reshape(seq_count, head_count, HD)
    key_heads = cache_keys.reshape(seq_count, position_index, head_count, HD)
    value_heads = cache_values.reshape(seq_count, position_index, head_count, HD)
    scores = (
        jnp.einsum("bhd,bphd->bhp", query_heads, key_heads, preferred_element_type=jnp.float32)
        * score_scale
    )
    scores = scores + forget[:, :, None] + cache_decay
    block_peak = jnp.max(scores, axis=2)
    raised = jnp.exp(scores - block_peak[:, :, None])
    block_total = jnp.sum(raised, axis=2)
    weighted = jnp.einsum(
        "bhp,bphd->bhd",
        raised.astype(jnp.bfloat16),
        value_heads,
        preferred_element_type=jnp.float32,
    )
    block_out = settle(weighted / block_total[:, :, None]).reshape(seq_count, head_count * HD)
    own_score = (
        jnp.einsum(
            "bhd,bhd->bh",
            query_heads,
            key_new.reshape(seq_count, head_count, HD),
            preferred_element_type=jnp.float32,
        )
        * score_scale
    )
    own_part = (own_score, jnp.ones_like(own_score), value_new.astype(jnp.float32))
    summit, weight_sum, out_sum = absorb(
        own_part,
        (
            lax.all_gather(block_peak[None].astype(jnp.bfloat16), "kv", axis=0, tiled=True).astype(
                jnp.float32
            ),
            lax.all_gather(block_total[None].astype(jnp.bfloat16), "kv", axis=0, tiled=True).astype(
                jnp.float32
            ),
            lax.all_gather(block_out[None].astype(jnp.bfloat16), "kv", axis=0, tiled=True).astype(
                jnp.float32
            ),
        ),
    )
    attended = (out_sum / spread_heads(weight_sum)).astype(jnp.bfloat16)
    projected = settle(jnp.dot(attended, output_weight, preferred_element_type=jnp.float32))
    mixed_block = lax.psum(projected.astype(jnp.bfloat16), "tp")
    mixed_rows = lax.all_gather(mixed_block, "kv", axis=1, tiled=True).astype(jnp.float32)
    after_mix = middle + root_norm(mixed_rows, norm_gains[3])
    second_sum = branch_total(
        gated_terms(after_mix, norm_gains[4], second_gate, second_lift, second_down)
    )
    own_rows = lax.dynamic_slice_in_dim(after_mix, own_start, own_width, 1)
    second_branch = lax.dynamic_slice_in_dim(
        root_norm(settle(second_sum), norm_gains[5]), own_start, own_width, 1
    )
    return (own_rows + 0.5 * second_branch).astype(jnp.bfloat16)


MESH = pl.DeviceIdType.MESH
F32 = jnp.float32
BF16 = jnp.bfloat16


def wide_dot(a, b):
    return lax.dot_general(a, b, (((1,), (1,)), ((), ())), preferred_element_type=F32)


def fused_kernel(n_kv, n_tp, *refs):
    n = n_kv * n_tp
    (tokens, gains, *hbm_refs) = refs[:16]
    out = refs[16]
    vmem_refs = refs[17:31]
    (
        x2d, stage, nrm, mid, stat, q2d, o2d, l2d,
        xbuf, send_all, recv_all, own_all, bbuf, mbuf, recv_two, tbuf,
        send_qkv, recv_qkv, own_kv, qbuf, send_part, recv_part,
        send_lse, recv_lse, abuf, send_tp, recv_tp,
        load_sem, all_send, all_recv, kv_send, kv_recv, tp_send, tp_recv,
    ) = refs[31:]
    (
        g1, l1, d1, wq, wk, wv, wf, wo, g2, l2, d2, ck, cv, cd
    ) = vmem_refs
    rows, c = tokens.shape
    depth = n * c
    kv = lax.axis_index("kv")
    tp = lax.axis_index("tp")
    me = kv * n_tp + tp

    order = (0, 1, 2, 3, 4, 5, 6, 11, 13, 12, 7, 8, 9, 10)
    loads = [
        pltpu.make_async_copy(hbm_refs[i], vmem_refs[i], load_sem.at[i]) for i in range(14)
    ]
    for i in order:
        loads[i].start()

    barrier = pltpu.get_barrier_semaphore()

    @pl.loop(1, n)
    def _(k):
        peer = lax.rem(me + k, n)
        pl.semaphore_signal(
            barrier, inc=1, device_id=(lax.div(peer, n_tp), lax.rem(peer, n_tp)),
            device_id_type=MESH,
        )

    pl.semaphore_wait(barrier, n - 1)

    def group(axis):
        if axis == "all":
            return n, me, lambda p: (lax.div(p, n_tp), lax.rem(p, n_tp)), all_send, all_recv
        if axis == "kv":
            return n_kv, kv, lambda p: (p, tp), kv_send, kv_recv
        return n_tp, tp, lambda p: (kv, p), tp_send, tp_recv

    def remote(src, dst, slot, axis, which, peer, index):
        size, here, place, send_sem, recv_sem = group(axis)
        return pltpu.make_async_remote_copy(
            src_ref=src, dst_ref=dst.at[slot],
            send_sem=send_sem.at[which, peer], recv_sem=recv_sem.at[which, index],
            device_id=place(peer), device_id_type=MESH,
        )

    def exchange(axis, pairs):
        size, here = group(axis)[:2]

        @pl.loop(1, size)
        def _(k):
            peer = lax.rem(here + k, size)
            for src, dst, which, scattered in pairs:
                remote(
                    src.at[peer] if scattered else src, dst, here, axis, which, peer, here
                ).start()

        for src, dst, which, scattered in pairs:
            dst[here] = src[here] if scattered else src[...]

        @pl.loop(1, size)
        def _(k):
            peer = lax.rem(here + k, size)
            for src, dst, which, scattered in pairs:
                remote(
                    src.at[peer] if scattered else src, dst, peer, axis, which, peer, peer
                ).wait()

    def flatten(buf, target, count):
        for i in range(count):
            target[:, i * c : (i + 1) * c] = buf[i].astype(target.dtype)

    def branch(pre_ref, gate, lift, down, first_load):
        for i in range(3):
            loads[first_load + i].wait()
        hidden = gate.shape[0]
        step = c * max(1, min(16, n))

        def up(k, carry):
            a, b = carry
            ds = pl.ds(pl.multiple_of(k * step, c), step)
            v = pre_ref[:, ds]
            a = a + wide_dot(v, gate[:, ds])
            b = b + wide_dot(v, lift[:, ds])
            return a, b

        zero = jnp.zeros((rows, hidden), F32)
        a, b = lax.fori_loop(0, depth // step, up, (zero, zero))
        active = (a / (1.0 + jnp.exp(-a)) * b).astype(BF16)
        group_size = step // c

        @pl.loop(0, depth // step)
        def _(k):
            ds = pl.ds(pl.multiple_of(k * step, c), step)
            y = jnp.dot(active, down[:, ds], preferred_element_type=F32).astype(BF16)
            for j in range(group_size):
                send_all[k * group_size + j] = y[:, j * c : (j + 1) * c]

    def total(buf, count):
        acc = buf[0].astype(F32)
        for i in range(1, count):
            acc = acc + buf[i].astype(F32)
        return acc

    exchange("all", [(tokens, xbuf, 0, False)])
    flatten(xbuf, x2d, n)
    nrm[...] = root_norm(x2d[...], gains[0:1, :]).astype(BF16)
    branch(nrm, g1, l1, d1, 0)
    exchange("all", [(send_all, recv_all, 1, True)])
    own_all[...] = total(recv_all, n).astype(BF16)
    exchange("all", [(own_all, bbuf, 2, False)])
    flatten(bbuf, stage, n)
    middle = x2d[...] + 0.5 * root_norm(stage[...], gains[1:2, :])
    mid[...] = middle
    nrm[...] = root_norm(middle, gains[2:3, :]).astype(BF16)

    for i in (3, 4, 5, 6):
        loads[i].wait()
    block_rows = wq.shape[0]
    block = nrm[:, pl.ds(pl.multiple_of(kv * block_rows, c), block_rows)]
    for i, w in enumerate((wq, wk, wv)):
        y = jnp.dot(block, w[...], preferred_element_type=F32).astype(BF16)
        for j in range(n_kv):
            send_qkv[j, i] = y[:, j * c : (j + 1) * c]
    forget_t = jax.nn.log_sigmoid(wide_dot(wf[...], nrm[...]))
    exchange("kv", [(send_qkv, recv_qkv, 0, True)])
    qkv = total(recv_qkv, n_kv).astype(BF16)
    own_kv[...] = qkv[0]
    exchange("kv", [(own_kv, qbuf, 1, False)])
    flatten(qbuf, q2d, n_kv)

    for i in (11, 12, 13):
        loads[i].wait()
    heads = wf.shape[0]
    width = heads * HD
    scale = HD ** (-0.5)
    head_of = lax.broadcasted_iota(jnp.int32, (heads, width), 1) // HD
    mask = head_of == lax.broadcasted_iota(jnp.int32, (heads, width), 0)

    lane = lax.broadcasted_iota(jnp.int32, (heads, rows), 1)
    pace = 3 if rows % 3 == 0 else 1

    def sequence(b):
        q = jnp.where(mask, q2d[pl.ds(b, 1), :], 0.0).astype(BF16)
        s = wide_dot(q, ck[b]) * scale + jnp.sum(
            jnp.where(lane == b, forget_t, 0.0), axis=1, keepdims=True
        ) + cd[b]
        peak = jnp.max(s, axis=1, keepdims=True)
        e = jnp.exp(s - peak)
        sums = jnp.sum(e, axis=1, keepdims=True)
        o = jnp.dot(e.astype(BF16), cv[b], preferred_element_type=F32) / sums
        lse = peak + jnp.log(sums)
        o2d[pl.ds(b, 1), :] = jnp.sum(jnp.where(mask, o, 0.0), axis=0, keepdims=True)
        l2d[pl.ds(b, 1), :] = jnp.sum(jnp.where(mask, lse, 0.0), axis=0, keepdims=True)

    @pl.loop(0, rows // pace)
    def _(k):
        for i in range(pace):
            sequence(k * pace + i)

    for j in range(n_kv):
        send_part[j] = o2d[:, j * c : (j + 1) * c].astype(BF16)
        send_lse[j] = l2d[:, j * c : (j + 1) * c]
    exchange("kv", [(send_part, recv_part, 2, True), (send_lse, recv_lse, 3, True)])
    qk = qkv[0].astype(F32) * qkv[1].astype(F32)
    lane_head = lax.broadcasted_iota(jnp.int32, (rows, c), 1) // HD
    own = jnp.zeros((rows, c), F32)
    for h in range(c // HD):
        mine = lane_head == h
        own = jnp.where(
            mine, jnp.sum(jnp.where(mine, qk, 0.0), axis=1, keepdims=True) * scale, own
        )
    top = own
    for j in range(n_kv):
        top = jnp.maximum(top, recv_lse[j])
    weight = jnp.exp(own - top)
    value = weight * qkv[2].astype(F32)
    for j in range(n_kv):
        w = jnp.exp(recv_lse[j] - top)
        weight = weight + w
        value = value + w * recv_part[j].astype(F32)
    own_kv[...] = (value / weight).astype(BF16)
    exchange("kv", [(own_kv, abuf, 4, False)])
    flatten(abuf, q2d, n_kv)
    loads[7].wait()
    y = jnp.dot(q2d[...].astype(BF16), wo[...], preferred_element_type=F32).astype(BF16)
    for j in range(n_tp):
        send_tp[j] = y[:, j * c : (j + 1) * c]
    exchange("tp", [(send_tp, recv_tp, 0, True)])
    own_all[...] = total(recv_tp, n_tp).astype(BF16)
    exchange("all", [(own_all, mbuf, 3, False)])
    flatten(mbuf, stage, n)
    after = mid[...] + root_norm(stage[...], gains[3:4, :])
    mid[...] = after
    nrm[...] = root_norm(after, gains[4:5, :]).astype(BF16)
    branch(nrm, g2, l2, d2, 8)
    exchange("all", [(send_all, recv_two, 4, True)])
    last = total(recv_two, n).astype(BF16)
    wide = last.astype(F32)
    diagonal = lax.broadcasted_iota(jnp.int32, (rows, c), 0) == lax.broadcasted_iota(
        jnp.int32, (rows, c), 1
    )
    row_sum = jnp.sum(wide * wide, axis=1, keepdims=True)
    stat[...] = jnp.sum(jnp.where(diagonal, row_sum, 0.0), axis=0, keepdims=True)
    exchange("all", [(stat, tbuf, 5, False)])
    squares = tbuf[0]
    for i in range(1, n):
        squares = squares + tbuf[i]
    row_sum = jnp.sum(jnp.where(diagonal, squares, 0.0), axis=1, keepdims=True)
    inv = lax.rsqrt(row_sum / depth + epsilon)
    here = pl.ds(pl.multiple_of(me * c, c), c)
    out[...] = (mid[:, here] + 0.5 * (last.astype(F32) * inv * gains[5:6, here])).astype(BF16)


def layer(n_kv, n_tp, *args):
    tokens = args[0]
    rows, c = tokens.shape
    n = n_kv * n_tp
    if c % 128 or rows > c or args[5].shape[1] != n_kv * c or args[9].shape[1] != n_tp * c:
        return body(*args)
    depth = n * c
    width = args[8].shape[1] * HD
    args = [a.T if i in (2, 3, 8, 10, 11) else a for i, a in enumerate(args)]
    vmem = pltpu.VMEM
    chunk = (rows, c)
    dma = pltpu.SemaphoreType.DMA
    scratch = [vmem(a.shape, a.dtype) for a in args[2:]]
    scratch += [
        vmem((rows, depth), F32),
        vmem((rows, depth), F32),
        vmem((rows, depth), BF16),
        vmem((rows, depth), F32),
        vmem((1, c), F32),
        vmem((rows, width), F32),
        vmem((rows, width), F32),
        vmem((rows, width), F32),
        vmem((n, *chunk), BF16),
        vmem((n, *chunk), BF16),
        vmem((n, *chunk), BF16),
        vmem(chunk, BF16),
        vmem((n, *chunk), BF16),
        vmem((n, *chunk), BF16),
        vmem((n, *chunk), BF16),
        vmem((n, 1, c), F32),
        vmem((n_kv, 3, *chunk), BF16),
        vmem((n_kv, 3, *chunk), BF16),
        vmem(chunk, BF16),
        vmem((n_kv, *chunk), BF16),
        vmem((n_kv, *chunk), BF16),
        vmem((n_kv, *chunk), BF16),
        vmem((n_kv, *chunk), F32),
        vmem((n_kv, *chunk), F32),
        vmem((n_kv, *chunk), BF16),
        vmem((n_tp, *chunk), BF16),
        vmem((n_tp, *chunk), BF16),
        dma((14,)),
        dma((6, n)),
        dma((6, n)),
        dma((5, n_kv)),
        dma((5, n_kv)),
        dma((1, n_tp)),
        dma((1, n_tp)),
    ]
    anywhere = pl.BlockSpec(memory_space=pl.ANY)
    inside = pl.BlockSpec(memory_space=pltpu.VMEM)
    return pl.pallas_call(
        functools.partial(fused_kernel, n_kv, n_tp),
        out_shape=jax.ShapeDtypeStruct((rows, c), BF16),
        in_specs=[inside, inside] + [anywhere] * 14,
        out_specs=inside,
        scratch_shapes=scratch,
        compiler_params=pltpu.CompilerParams(
            collective_id=0, has_side_effects=True, vmem_limit_bytes=66 * 1000 * 1000
        ),
    )(*args)


def solution(mesh):
    return jax.shard_map(
        functools.partial(layer, mesh.shape["kv"], mesh.shape["tp"]),
        mesh=mesh,
        in_specs=(
            P(None, ("kv", "tp")),
            P(),
            P(None, ("kv", "tp")),
            P(None, ("kv", "tp")),
            P(("kv", "tp"), None),
            P("kv", "tp"),
            P("kv", "tp"),
            P("kv", "tp"),
            P(None, "tp"),
            P("tp", "kv"),
            P(None, ("kv", "tp")),
            P(None, ("kv", "tp")),
            P(("kv", "tp"), None),
            P(None, "kv", "tp"),
            P(None, "kv", "tp"),
            P(None, "tp", "kv"),
        ),
        out_specs=P(None, ("kv", "tp")),
        check_vma=False,
    )
```
